32 devices in a mesh: sp: 8 (over z, y), tp: 4 (over x, core).
Axes of the slice: x: 2, y: 2, z: 4, core: 2. Of those that a mesh axis runs over, the one named last changes fastest.
Arguments:
- skip_stream: bfloat16 [2048, 2048], P('sp', 'tp'), may hold values from -20 to 20
- narrow_lookup_matrix: bfloat16 [2048, 256], P('sp', 'tp'), may hold values from -6 to 6
- narrow_probe_matrix: bfloat16 [2048, 256], P('sp', 'tp'), may hold values from -6 to 6
- narrow_retention_logits: bfloat16 [2048, 256], P('sp', 'tp'), may hold values from -6 to 16
- broad_lookup_matrix: bfloat16 [2048, 512], P('sp', 'tp'), may hold values from -6 to 6
- broad_probe_matrix: bfloat16 [2048, 512], P('sp', 'tp'), may hold values from -6 to 6
- broad_retention_logits: bfloat16 [2048, 512], P('sp', 'tp'), may hold values from -6 to 16
- content_vectors: bfloat16 [2048, 4, 2, 128], P('sp', 'tp'), may hold values from -6 to 6
- extra_log_retention: float32 [2048, 2, 4], P('sp', None, 'tp'), may hold values from -0.7 to 0
- per_branch_scaling: bfloat16 [4, 2, 128], P('tp'), may hold values from 0.099609375 to 1.8984375
- final_projection_matrix: bfloat16 [1024, 2048], P(None, 'tp'), may hold values from -0.1875 to 0.1875
- channel_blend_scaling: bfloat16 [2048], replicated, may hold values from 0.099609375 to 1.8984375
- switch_expansion_matrix: bfloat16 [2048, 5632], P('sp', 'tp'), may hold values from -0.125 to 0.125
- content_expansion_matrix: bfloat16 [2048, 5632], P('sp', 'tp'), may hold values from -0.125 to 0.125
- convolution_kernel: bfloat16 [3, 2, 5632], P(None, None, 'tp'), may hold values from -3.5 to 3.5
- contraction_matrix: bfloat16 [5632, 2048], P('tp', 'sp'), may hold values from -0.078125 to 0.078125
Outputs:
- mixed: bfloat16 [2048, 2048], P('sp', 'tp')
The draws below stay inside these ranges and needn't reach their ends.
All inputs are finite; a program needn't handle non-finite values.
Results may differ from the reference program's by a relative error of at most 0.011.
Values may be sent and summed in bfloat16 or wider, within the bound.
A program may use at most 64 MiB of HBM per device.

```python
import jax
import jax.numpy as jnp
from jax import lax

D = 2048
FF = 5632
GROUP_HEADS = 4
NARROW_PROBE_DIM = 64
BROAD_PROBE_DIM = 128
DV = 128
BLOCK = 64
TOK_DEV = 256
TOKENS = 2048
N_TP = 4


def decay_draw(key, model_width):
    subkeys = jax.random.split(key, 5)
    slow_share = 0.5
    slow = jax.random.uniform(subkeys[0], (GROUP_HEADS,)) < slow_share
    slow_rate = jnp.log(10.0) / TOKENS * jax.random.uniform(subkeys[1], (GROUP_HEADS,), minval=0.05, maxval=0.2)
    fast_rate = jax.random.uniform(subkeys[2], (GROUP_HEADS,), minval=0.01, maxval=0.033)
    rate = jnp.where(slow, slow_rate, fast_rate)
    factor = jnp.exp(jax.random.uniform(subkeys[3], (TOKENS // TOK_DEV,), minval=-0.7, maxval=0.7))
    factor = jnp.repeat(factor, TOK_DEV)
    noise = jnp.exp(0.5 * jnp.clip(jax.random.normal(subkeys[4], (TOKENS, GROUP_HEADS, model_width)), -3.0, 3.0))
    strength = rate[None, :, None] * factor[:, None, None] * noise
    preact = -jnp.log(jnp.expm1(16.0 * strength))
    return preact.reshape(TOKENS, GROUP_HEADS * model_width).astype(jnp.bfloat16)


def draw_narrow_retention_logits(key, part):
    return decay_draw(jax.random.fold_in(key, 11), NARROW_PROBE_DIM)


def draw_broad_retention_logits(key, part):
    return decay_draw(jax.random.fold_in(key, 13), BROAD_PROBE_DIM)


def draw_extra_log_retention(key, part):
    subkeys = jax.random.split(jax.random.fold_in(key, 31), 2)
    spots = jax.random.randint(subkeys[0], (4,), 0, TOKENS)
    places = jnp.arange(TOKENS)
    struck = jnp.any(places[:, None] == spots[None, :], axis=1)
    losses = jnp.log(jax.random.uniform(subkeys[1], (TOKENS, 2, GROUP_HEADS), minval=0.5, maxval=0.8))
    return jnp.where(struck[:, None, None], losses, 0.0).astype(jnp.float32)


def draw_skip_stream(key, part):
    subkey = jax.random.fold_in(key, 47)
    column = jnp.arange(D, dtype=jnp.float32) / D
    entries = jnp.clip(jax.random.normal(subkey, (TOKENS, D)), -6.0, 6.0)
    ramp = jnp.exp(jnp.log(3.0) * column)
    return (entries * ramp[None, :]).astype(jnp.bfloat16)


def block_scale(own_key, extent, pieces, smallest, largest):
    level, own = 1.0, jax.random.fold_in(own_key, 6)
    for axis_at, shards_of in pieces:
        draws = jnp.exp(jax.random.uniform(jax.random.fold_in(own, axis_at), (shards_of,), jnp.float32, smallest / len(pieces), largest / len(pieces)))
        level = level * jnp.repeat(draws, extent[axis_at] // shards_of).reshape([-1 if axis == axis_at else 1 for axis in range(len(extent))])
    return level


def scatter_about(rng, extent, spread, reach, pieces=(), kind=jnp.bfloat16):
    values = spread * jax.random.normal(rng, extent, jnp.float32)
    if pieces:
        values = values * block_scale(rng, extent, pieces, -0.22, 0.18)
    return jnp.clip(values, -reach, reach).astype(kind)


def setup_inputs(seed: int = 0) -> dict:
    splits = jax.random.split(jax.random.key(seed), 17)
    return {
        "skip_stream": draw_skip_stream(jax.random.fold_in(splits[16], 71), 0),
        "narrow_lookup_matrix": scatter_about(splits[1], (TOKENS, GROUP_HEADS * NARROW_PROBE_DIM), 1.0, 6.0, ((0, 8), (1, 4))),
        "narrow_probe_matrix": scatter_about(splits[2], (TOKENS, GROUP_HEADS * NARROW_PROBE_DIM), 1.0, 6.0, ((0, 8), (1, 4))),
        "narrow_retention_logits": draw_narrow_retention_logits(jax.random.fold_in(splits[16], 71), 0),
        "broad_lookup_matrix": scatter_about(splits[4], (TOKENS, GROUP_HEADS * BROAD_PROBE_DIM), 1.0, 6.0, ((0, 8), (1, 4))),
        "broad_probe_matrix": scatter_about(splits[5], (TOKENS, GROUP_HEADS * BROAD_PROBE_DIM), 1.0, 6.0, ((0, 8), (1, 4))),
        "broad_retention_logits": draw_broad_retention_logits(jax.random.fold_in(splits[16], 71), 0),
        "content_vectors": scatter_about(splits[7], (TOKENS, GROUP_HEADS, 2, DV), 1.0, 6.0, ((0, 8), (1, 4))),
        "extra_log_retention": draw_extra_log_retention(jax.random.fold_in(splits[16], 71), 0),
        "per_branch_scaling": jnp.clip(1.0 + 0.18 * jax.random.normal(splits[9], (GROUP_HEADS, 2, DV), jnp.float32), 0.099609375, 1.8984375).astype(jnp.bfloat16),
        "final_projection_matrix": scatter_about(splits[10], (2 * GROUP_HEADS * DV, D), (2 * GROUP_HEADS * DV) ** -0.5, 0.1875, ((1, 4),)),
        "channel_blend_scaling": jnp.clip(1.0 + 0.18 * jax.random.normal(splits[11], (D,), jnp.float32), 0.099609375, 1.8984375).astype(jnp.bfloat16),
        "switch_expansion_matrix": scatter_about(splits[12], (D, FF), D ** -0.5, 0.125, ((0, 8), (1, 4))),
        "content_expansion_matrix": scatter_about(splits[13], (D, FF), D ** -0.5, 0.125, ((0, 8), (1, 4))),
        "convolution_kernel": scatter_about(splits[14], (3, 2, FF), 3 ** -0.5, 3.5, ((2, 4),)),
        "contraction_matrix": scatter_about(splits[15], (FF, D), FF ** -0.5, 0.078125, ((0, 4), (1, 8))),
    }


EPSILON = 1e-06
SOFTENING = 16.0
HIGHEST = lax.Precision.HIGHEST

def blocked(array):
    return array.reshape(array.shape[0] // BLOCK, BLOCK, array.shape[1], array.shape[2]).transpose(0, 2, 1, 3)

def gla_group(query_rows, input_keys, values_in, log_decay):
    query_blocks = blocked(query_rows)
    key_blocks = blocked(input_keys)
    value_blocks = blocked(values_in)
    inner = jnp.cumsum(blocked(log_decay), axis=2)
    last = inner[:, :, -1:, :]
    middle = inner[:, :, BLOCK // 2 - 1:BLOCK // 2, :]
    scores = jnp.einsum('nhid,nhjd->nhij', query_blocks * jnp.exp(inner - middle), key_blocks * jnp.exp(middle - inner), precision=HIGHEST)
    lower = jnp.tril(jnp.ones((BLOCK, BLOCK), dtype=bool))
    local_out = jnp.einsum('nhij,nhjv->nhiv', jnp.where(lower, scores, 0.0), value_blocks, precision=HIGHEST)
    query_carry = query_blocks * jnp.exp(inner)
    key_carry = key_blocks * jnp.exp(last - inner)
    fade = jnp.exp(last[:, :, 0, :])

    def advance(state, inputs):
        query_part, key_part, value_part, fade_part = inputs
        output = jnp.einsum('hid,hdv->hiv', query_part, state, precision=HIGHEST)
        state = fade_part[..., None] * state + jnp.einsum('hjd,hjv->hdv', key_part, value_part, precision=HIGHEST)
        return (state, output)
    start = jnp.zeros((query_blocks.shape[1], query_blocks.shape[3], value_blocks.shape[3]), jnp.float32)
    _, carried = lax.scan(advance, start, (query_carry, key_carry, value_blocks, fade))
    total = local_out + carried
    return total.transpose(0, 2, 1, 3).reshape(query_rows.shape[0], total.shape[1], total.shape[3])

def head_norm(output, gain):
    scale = lax.rsqrt(lax.optimization_barrier(jnp.mean(output * output, axis=-1, keepdims=True)) + EPSILON)
    return output * scale * gain.astype(jnp.float32)

def build_arguments(query_rows, input_keys, forget_gates, spike_column, model_width):
    item_count = query_rows.shape[0]
    query_data = query_rows.astype(jnp.float32).reshape(item_count, GROUP_HEADS, model_width) * model_width ** (-0.5)
    key_data = input_keys.astype(jnp.float32).reshape(item_count, GROUP_HEADS, model_width)
    decay_factor = jax.nn.log_sigmoid(forget_gates.astype(jnp.float32).reshape(item_count, GROUP_HEADS, model_width)) / SOFTENING + spike_column[:, :, None]
    return (query_data, key_data, decay_factor)

def reference(skip_stream, narrow_lookup_matrix, narrow_probe_matrix, narrow_retention_logits, broad_lookup_matrix, broad_probe_matrix, broad_retention_logits, content_vectors, extra_log_retention, per_branch_scaling, final_projection_matrix, channel_blend_scaling, switch_expansion_matrix, content_expansion_matrix, convolution_kernel, contraction_matrix):
    item_count = skip_stream.shape[0]
    value_data = content_vectors.astype(jnp.float32)
    narrow_lookup_vector, narrow_probe_vector, narrow_probe_dim = build_arguments(narrow_lookup_matrix, narrow_probe_matrix, narrow_retention_logits, extra_log_retention[:, 0], NARROW_PROBE_DIM)
    broad_lookup_vector, broad_probe_vector, broad_probe_dim = build_arguments(broad_lookup_matrix, broad_probe_matrix, broad_retention_logits, extra_log_retention[:, 1], BROAD_PROBE_DIM)
    out_small = gla_group(narrow_lookup_vector, narrow_probe_vector, value_data[:, :, 0], narrow_probe_dim)
    out_large = gla_group(broad_lookup_vector, broad_probe_vector, value_data[:, :, 1], broad_probe_dim)
    stacked = jnp.stack([head_norm(out_small, per_branch_scaling[:, 0]), head_norm(out_large, per_branch_scaling[:, 1])], axis=2)
    heads_in = stacked.reshape(item_count, 2 * GROUP_HEADS * DV).astype(jnp.bfloat16)
    resid = (skip_stream.astype(jnp.float32) + jnp.dot(heads_in, final_projection_matrix, preferred_element_type=jnp.float32)).astype(jnp.bfloat16)
    resid_data = resid.astype(jnp.float32)
    scale = lax.rsqrt(lax.optimization_barrier(jnp.mean(resid_data * resid_data, axis=1, keepdims=True)) + EPSILON)
    normed = (resid_data * scale * channel_blend_scaling.astype(jnp.float32)).astype(jnp.bfloat16)
    padded = jnp.concatenate([jnp.zeros((2, normed.shape[1]), jnp.bfloat16), normed], axis=0)
    taps = convolution_kernel.astype(jnp.float32)
    group_width = FF // N_TP

    def convolve(upward, tap_rows):
        return tap_rows[0] * upward[:-2] + tap_rows[1] * upward[1:-1] + tap_rows[2] * upward[2:]

    def mixer_block(index):
        start = (index * TOK_DEV).astype(jnp.int32)
        window = lax.dynamic_slice_in_dim(padded, start, TOK_DEV + 2, 0)
        up_gate = lax.optimization_barrier(jnp.dot(window, switch_expansion_matrix, preferred_element_type=jnp.float32).astype(jnp.bfloat16)).astype(jnp.float32)
        up_value = lax.optimization_barrier(jnp.dot(window, content_expansion_matrix, preferred_element_type=jnp.float32).astype(jnp.bfloat16)).astype(jnp.float32)
        conv_gate = convolve(up_gate, taps[:, 1])
        conv_value = convolve(up_value, taps[:, 0])
        hidden = (jax.nn.silu(conv_gate) * conv_value).astype(jnp.bfloat16)
        summed = jnp.zeros((TOK_DEV, contraction_matrix.shape[1]), jnp.float32)
        for group in range(N_TP):
            partial_product = jnp.dot(hidden[:, group * group_width:(group + 1) * group_width], contraction_matrix[group * group_width:(group + 1) * group_width], preferred_element_type=jnp.float32)
            summed = summed + lax.optimization_barrier(partial_product.astype(jnp.bfloat16)).astype(jnp.float32)
        return summed
    downs = lax.map(mixer_block, jnp.arange(item_count // TOK_DEV, dtype=jnp.int32))
    down = downs.reshape(item_count, contraction_matrix.shape[1])
    return (resid_data + down).astype(jnp.bfloat16)
```

```python
import functools

import jax
import jax.numpy as jnp
from jax import lax
from jax.experimental import pallas as pl
from jax.experimental.pallas import tpu as pltpu
from jax.sharding import PartitionSpec as P

BLOCK = 64
HALO = 16
EPSILON = 1e-06
SOFTENING = 16.0
HIGHEST = lax.Precision.HIGHEST
F32 = jnp.float32
BF16 = jnp.bfloat16
NT = (((1,), (1,)), ((), ()))


def blocked(array):
    return array.reshape(array.shape[0] // BLOCK, BLOCK, array.shape[1], array.shape[2]).transpose(
        0, 2, 1, 3
    )


def local_attention(q, k, v, log_decay):
    tokens, units, key = q.shape
    query_blocks, key_blocks, value_blocks = blocked(q), blocked(k), blocked(v)
    lower = jnp.tril(jnp.ones((BLOCK, BLOCK), dtype=bool))
    inner = jnp.einsum(
        "ij,nhjd->nhid", lower.astype(F32), blocked(log_decay), precision=HIGHEST
    )
    last = inner[:, :, -1:, :]
    middle = inner[:, :, BLOCK // 2 - 1 : BLOCK // 2, :]
    scores = jnp.einsum(
        "nhid,nhjd->nhij",
        query_blocks * jnp.exp(inner - middle),
        key_blocks * jnp.exp(middle - inner),
        precision=HIGHEST,
    )
    out = jnp.einsum(
        "nhij,nhjv->nhiv", jnp.where(lower, scores, 0.0), value_blocks, precision=HIGHEST
    )
    query_carry = query_blocks * jnp.exp(inner)
    key_carry = key_blocks * jnp.exp(last - inner)
    added = jnp.einsum("nhjd,nhjv->nhvd", key_carry, value_blocks, precision=HIGHEST)
    block_logs = last[:, :, 0, :]
    before = jnp.cumsum(block_logs, axis=0) - block_logs
    state, states = jnp.zeros_like(added[0]), []
    for n in range(added.shape[0]):
        states.append(state)
        state = jnp.exp(block_logs[n])[:, None, :] * state + added[n]
    out = out + jnp.einsum("nhid,nhvd->nhiv", query_carry, jnp.stack(states), precision=HIGHEST)
    meets = query_carry * jnp.exp(before)[:, :, None, :]
    fade = jnp.exp(jnp.sum(block_logs, axis=0))

    def unblock(a):
        return a.transpose(0, 2, 1, 3).reshape(tokens, -1)

    return unblock(out), unblock(meets), state, fade


def kernel(
    n_sp, n_tp, units,
    w_ref, st_ref, out_ref0, meets_ref, gain_ref, skip_ref, proj_ref, blend_ref, taps_ref,
    mixed_ref,
    wbuf, stbuf, acc_state, heads, resid, nb, up, hid, psum, rbuf,
    own_sem, st_send, st_recv, uz_send, uz_recv, uy_send, uy_recv, cz_send, cz_recv, cy_send,
    cy_recv, h_send, h_recv, r_send, r_recv, n_send, n_recv, d_send, d_recv,
):
    s, t = lax.axis_index("sp"), lax.axis_index("tp")
    nz = n_sp // 2
    z, y = s // 2, s % 2
    q = z % 2
    mate = s + 2 - 4 * q
    side = s + 1 - 2 * y
    tok = skip_ref.shape[0]
    cols = skip_ref.shape[1]
    half = wbuf.shape[2]
    dblk = wbuf.shape[3]
    dv = out_ref0.shape[1] // units

    def rc(src, dst, ss, rs, sp, tp):
        return pltpu.make_async_remote_copy(
            src_ref=src, dst_ref=dst, send_sem=ss, recv_sem=rs,
            device_id=(sp, tp), device_id_type=pl.DeviceIdType.MESH,
        )

    bar = pltpu.get_barrier_semaphore()
    count = 0
    for o in range(1, n_sp):
        pl.semaphore_signal(bar, inc=1, device_id=(lax.rem(s + o, n_sp), t),
                            device_id_type=pl.DeviceIdType.MESH)
        count += 1
    for row in (s, mate):
        for o in range(1, n_tp):
            pl.semaphore_signal(bar, inc=1, device_id=(row, lax.rem(t + o, n_tp)),
                                device_id_type=pl.DeviceIdType.MESH)
            count += 1
    pl.semaphore_wait(bar, count)

    st = [None] + [
        rc(st_ref, stbuf.at[s], st_send.at[o], st_recv.at[o], lax.rem(s + o, n_sp), t)
        for o in range(1, n_sp)
    ]
    for o in range(1, n_sp):
        @pl.when(s + o < n_sp)
        def _(o=o):
            st[o].start()

    def zcopies(lo, width, ss, rs):
        made = []
        for o in range(1, nz):
            zz = lax.rem(z + o, nz)
            rows = pl.ds(pl.multiple_of((zz % 2) * half, HALO), half)
            made.append(rc(w_ref.at[pl.ds(lo, width), rows], wbuf.at[s, pl.ds(lo, width)],
                           ss.at[o], rs.at[o], zz * 2 + y, t))
        return made

    def ycopy(o, lo, width, ss, rs):
        if o == 0:
            rows = pl.ds(pl.multiple_of(q * half, HALO), half)
            source = w_ref.at[pl.ds(lo, width), rows]
            slot = s
        else:
            slot = lax.rem(z + nz - o, nz) * 2 + y
            source = wbuf.at[slot, pl.ds(lo, width)]
        return rc(source, wbuf.at[slot, pl.ds(lo, width)], ss.at[o], rs.at[o], side, t)

    uz = zcopies(0, 2, uz_send, uz_recv)
    uy = [ycopy(o, 0, 2, uy_send, uy_recv) for o in range(nz)]
    for copy in uz:
        copy.start()
    uy[0].start()
    own = pltpu.make_async_copy(
        w_ref.at[:, pl.ds(pl.multiple_of(q * half, HALO), half)], wbuf.at[s], own_sem
    )
    own.start()

    acc_state[...] = jnp.zeros_like(acc_state)
    for o in range(n_sp - 1, 0, -1):
        @pl.when(s - o >= 0)
        def _(o=o):
            st[o].wait_recv()
            got = stbuf[s - o].astype(F32)
            acc_state[...] = got[dv : dv + 1] * acc_state[...] + got[:dv]
    key = meets_ref.shape[1] // units
    mine = []
    for u in range(units):
        total = out_ref0[:, u * dv : (u + 1) * dv] + lax.dot_general(
            meets_ref[:, u * key : (u + 1) * key], acc_state[:, u * key : (u + 1) * key],
            NT, precision=HIGHEST, preferred_element_type=F32,
        )
        scale = lax.rsqrt(jnp.mean(total * total, axis=-1, keepdims=True) + EPSILON)
        mine.append((total * scale * gain_ref[u : u + 1, :]).astype(BF16))
    heads[t] = jnp.concatenate(mine, axis=1)
    hc = [
        rc(heads.at[t], heads.at[t], h_send.at[o], h_recv.at[o], s, lax.rem(t + o, n_tp))
        for o in range(1, n_tp)
    ]
    for copy in hc:
        copy.start()
    for copy in hc:
        copy.wait_recv()
    width = units * dv
    projected = skip_ref[...].astype(F32)
    whole_heads = jnp.concatenate([heads[i] for i in range(n_tp)], axis=1)
    projected = projected + jnp.dot(whole_heads, proj_ref[...], preferred_element_type=F32)
    resid[t] = projected.astype(BF16)
    qc = [
        rc(resid.at[t], resid.at[t], r_send.at[o], r_recv.at[o], s, lax.rem(t + o, n_tp))
        for o in range(1, n_tp)
    ]
    for copy in qc:
        copy.start()
    for copy in qc:
        copy.wait_recv()
    squares = jnp.zeros((tok, 1), F32)
    for i in range(n_tp):
        part = resid[i].astype(F32)
        squares = squares + jnp.sum(part * part, axis=1, keepdims=True)
    scale = lax.rsqrt(squares / (n_tp * cols) + EPSILON)
    for i in range(n_tp):
        piece = slice(i * cols, (i + 1) * cols)
        nb[0, HALO:, piece] = (
            resid[i].astype(F32) * scale * blend_ref[:, piece]
        ).astype(BF16)
    after = lax.rem(s + 1, n_sp)
    after_mate = after + 2 - 4 * ((after // 2) % 2)
    block = pl.ds(HALO, tok)
    tail = pl.ds(tok, HALO)
    nc = [
        rc(nb.at[0, tail], nb.at[0, pl.ds(0, HALO)], n_send.at[0], n_recv.at[0], after, t),
        rc(nb.at[0, tail], nb.at[1, pl.ds(0, HALO)], n_send.at[1], n_recv.at[1], after_mate, t),
        rc(nb.at[0, block], nb.at[1, block], n_send.at[2], n_recv.at[2], mate, t),
    ]
    for copy in nc:
        copy.start()
    cz = zcopies(2, 1, cz_send, cz_recv)
    cy = [ycopy(o, 2, 1, cy_send, cy_recv) for o in range(nz)]
    for copy in cz:
        copy.start()
    for o in range(1, nz):
        uz[o - 1].wait_recv()
        uy[o].start()
    cy[0].start()
    for copy in nc:
        copy.wait_recv()
    own.wait()
    for o in range(nz):
        uy[o].wait_recv()

    for m in range(2):
        for i in range(2):
            up[m, i] = jnp.zeros_like(up[m, i])

    group = max(1, 128 // dblk)

    def expand_add(b, carry):
        at = pl.ds(pl.multiple_of(b * group * dblk, 128), group * dblk)
        for i in range(2):
            rows = nb[i, :, at]
            for j in range(group):
                part = rows[:, j * dblk : (j + 1) * dblk]
                for m in range(2):
                    up[m, i] += lax.dot_general(
                        part, wbuf[b * group + j, m], NT, preferred_element_type=F32
                    )
        return carry

    lax.fori_loop(0, n_sp // group, expand_add, 0)
    for o in range(1, nz):
        cz[o - 1].wait_recv()
        cy[o].start()
    for i in range(2):
        first = (s if i == 0 else mate) == 0
        conv = []
        for m in range(2):
            keep = jnp.where(first, 0.0, 1.0)
            edge = up[m, i, :HALO].astype(BF16).astype(F32)
            up[m, i, :HALO] = edge * keep
            up[m, i, HALO:] = up[m, i, HALO:].astype(BF16).astype(F32)
            total = taps_ref[m * 3 : m * 3 + 1] * up[m, i, pl.ds(HALO - 2, tok)]
            total += taps_ref[m * 3 + 1 : m * 3 + 2] * up[m, i, pl.ds(HALO - 1, tok)]
            total += taps_ref[m * 3 + 2 : m * 3 + 3] * up[m, i, pl.ds(HALO, tok)]
            conv.append(total)
        value, gate = conv
        hid[pl.ds(i * tok, tok)] = (gate / (1.0 + jnp.exp(-gate)) * value).astype(BF16)
    for o in range(nz):
        cy[o].wait_recv()
    per = cols // dblk
    dc = []
    for o in range(1, n_tp + 1):
        to = lax.rem(t + o, n_tp)
        for j in range(per):
            part = jnp.dot(hid[...], wbuf[to * per + j, 2], preferred_element_type=F32).astype(BF16)
            psum[to, 0, :, j * dblk : (j + 1) * dblk] = part[:tok]
            psum[to, 1, :, j * dblk : (j + 1) * dblk] = part[tok:]
        for i in range(2):
            if i == 0 and o == n_tp:
                continue
            at = i * n_tp + o - 1
            copy = rc(psum.at[to, i], rbuf.at[at], d_send.at[at], d_recv.at[at],
                      s if i == 0 else mate, to)
            copy.start()
            dc.append((at, copy))
    total = psum[t, 0].astype(F32)
    for at, copy in dc:
        copy.wait_recv()
        total = total + rbuf[at].astype(F32)
    mixed_ref[...] = (resid[t].astype(F32) + total).astype(BF16)

    for o in range(1, n_sp):
        @pl.when(s + o < n_sp)
        def _(o=o):
            st[o].wait_send()
    for copy in uz + uy + cz + cy + hc + qc + nc + [c for _, c in dc]:
        copy.wait_send()


def local(
    n_sp, n_tp,
    skip_stream,
    narrow_lookup_matrix,
    narrow_probe_matrix,
    narrow_retention_logits,
    broad_lookup_matrix,
    broad_probe_matrix,
    broad_retention_logits,
    content_vectors,
    extra_log_retention,
    per_branch_scaling,
    final_projection_matrix,
    channel_blend_scaling,
    switch_expansion_matrix,
    content_expansion_matrix,
    convolution_kernel,
    contraction_matrix,
):
    tok, cols = skip_stream.shape
    heads = content_vectors.shape[1]
    dv = content_vectors.shape[3]
    narrow = narrow_lookup_matrix.shape[1] // heads
    broad = broad_lookup_matrix.shape[1] // heads
    units = 2 * heads

    def pair(a, b):
        a = a.astype(F32).reshape(tok, heads, narrow)
        b = b.astype(F32).reshape(tok, heads, broad)
        return a, b

    def join(a, b):
        a = jnp.pad(a, ((0, 0), (0, 0), (0, broad - narrow)))
        return jnp.stack([a, b], axis=2).reshape(tok, units, broad)

    qa, qb = pair(narrow_lookup_matrix, broad_lookup_matrix)
    query = join(qa * narrow ** (-0.5), qb * broad ** (-0.5))
    keys = join(*pair(narrow_probe_matrix, broad_probe_matrix))
    gates = join(*pair(narrow_retention_logits, broad_retention_logits))
    extra = extra_log_retention.transpose(0, 2, 1).reshape(tok, units, 1)
    decay = jax.nn.log_sigmoid(gates) / SOFTENING + extra
    values = content_vectors.astype(F32).reshape(tok, units, dv)
    out, meets, state, fade = local_attention(query, keys, values, decay)
    packed = jnp.concatenate(
        [
            state.transpose(1, 0, 2).reshape(dv, units * broad),
            fade.reshape(1, units * broad),
            jnp.zeros((15, units * broad), F32),
        ],
        axis=0,
    ).astype(BF16)
    weights = jnp.stack(
        [content_expansion_matrix.T, switch_expansion_matrix.T, contraction_matrix], axis=0
    )
    ff = contraction_matrix.shape[0]
    half = ff // 2
    dblk = contraction_matrix.shape[1]
    q = (lax.axis_index("sp") // 2) % 2
    taps = lax.dynamic_slice_in_dim(convolution_kernel, q * half, half, axis=2)
    taps = jnp.pad(taps.astype(F32).transpose(1, 0, 2).reshape(6, half), ((0, 2), (0, 0)))
    gain = per_branch_scaling.astype(F32).reshape(units, dv)
    blend = channel_blend_scaling.astype(F32).reshape(1, -1)
    nz = n_sp // 2
    model = n_tp * cols
    dma = pltpu.SemaphoreType.DMA
    vmem = pl.BlockSpec(memory_space=pltpu.VMEM)
    return pl.pallas_call(
        functools.partial(kernel, n_sp, n_tp, units),
        out_shape=jax.ShapeDtypeStruct((tok, cols), BF16),
        in_specs=[vmem] * 9,
        out_specs=vmem,
        scratch_shapes=[
            pltpu.VMEM((n_sp, 3, half, dblk), BF16),
            pltpu.VMEM((n_sp,) + packed.shape, BF16),
            pltpu.VMEM((dv, units * broad), F32),
            pltpu.VMEM((n_tp, tok, units * dv), BF16),
            pltpu.VMEM((n_tp, tok, cols), BF16),
            pltpu.VMEM((2, tok + HALO, model), BF16),
            pltpu.VMEM((2, 2, tok + HALO, half), F32),
            pltpu.VMEM((2 * tok, half), BF16),
            pltpu.VMEM((n_tp, 2, tok, cols), BF16),
            pltpu.VMEM((2 * n_tp, tok, cols), BF16),
            dma,
            dma((n_sp,)), dma((n_sp,)),
            dma((nz,)), dma((nz,)), dma((nz,)), dma((nz,)),
            dma((nz,)), dma((nz,)), dma((nz,)), dma((nz,)),
            dma((n_tp,)), dma((n_tp,)), dma((n_tp,)), dma((n_tp,)),
            dma((3,)), dma((3,)), dma((2 * n_tp,)), dma((2 * n_tp,)),
        ],
        compiler_params=pltpu.CompilerParams(
            collective_id=0, has_side_effects=True, vmem_limit_bytes=56 * 1024 * 1024
        ),
    )(weights, packed, out, meets, gain, skip_stream, final_projection_matrix, blend, taps)


def solution(mesh):
    in_specs = (
        P("sp", "tp"),
        P("sp", "tp"),
        P("sp", "tp"),
        P("sp", "tp"),
        P("sp", "tp"),
        P("sp", "tp"),
        P("sp", "tp"),
        P("sp", "tp", None, None),
        P("sp", None, "tp"),
        P("tp", None, None),
        P(None, "tp"),
        P(),
        P("sp", "tp"),
        P("sp", "tp"),
        P(None, None, "tp"),
        P("tp", "sp"),
    )
    out_specs = P("sp", "tp")
    body = functools.partial(local, mesh.shape["sp"], mesh.shape["tp"])
    return jax.shard_map(body, mesh=mesh, in_specs=in_specs, out_specs=out_specs, check_vma=False)
```

```python
import functools

import jax
import jax.numpy as jnp
from jax import lax
from jax.experimental import pallas as pl
from jax.experimental.pallas import tpu as pltpu
from jax.sharding import PartitionSpec as P

BLOCK = 64
HALO = 16
EPSILON = 1e-06
SOFTENING = 16.0
HIGHEST = lax.Precision.HIGHEST
F32 = jnp.float32
BF16 = jnp.bfloat16
NT = (((1,), (1,)), ((), ()))


def blocked(array):
    return array.reshape(array.shape[0] // BLOCK, BLOCK, array.shape[1], array.shape[2]).transpose(
        0, 2, 1, 3
    )


def local_attention(q, k, v, log_decay):
    tokens, units, key = q.shape
    query_blocks, key_blocks, value_blocks = blocked(q), blocked(k), blocked(v)
    lower = jnp.tril(jnp.ones((BLOCK, BLOCK), dtype=bool))
    inner = jnp.einsum(
        "ij,nhjd->nhid", lower.astype(F32), blocked(log_decay), precision=HIGHEST
    )
    last = inner[:, :, -1:, :]
    middle = inner[:, :, BLOCK // 2 - 1 : BLOCK // 2, :]
    scores = jnp.einsum(
        "nhid,nhjd->nhij",
        query_blocks * jnp.exp(inner - middle),
        key_blocks * jnp.exp(middle - inner),
        precision=HIGHEST,
    )
    out = jnp.einsum(
        "nhij,nhjv->nhiv", jnp.where(lower, scores, 0.0), value_blocks, precision=HIGHEST
    )
    query_carry = query_blocks * jnp.exp(inner)
    key_carry = key_blocks * jnp.exp(last - inner)
    added = jnp.einsum("nhjd,nhjv->nhvd", key_carry, value_blocks, precision=HIGHEST)
    block_logs = last[:, :, 0, :]
    before = jnp.cumsum(block_logs, axis=0) - block_logs
    state, states = jnp.zeros_like(added[0]), []
    for n in range(added.shape[0]):
        states.append(state)
        state = jnp.exp(block_logs[n])[:, None, :] * state + added[n]
    out = out + jnp.einsum("nhid,nhvd->nhiv", query_carry, jnp.stack(states), precision=HIGHEST)
    meets = query_carry * jnp.exp(before)[:, :, None, :]
    fade = jnp.exp(jnp.sum(block_logs, axis=0))

    def unblock(a):
        return a.transpose(0, 2, 1, 3).reshape(tokens, -1)

    return unblock(out), unblock(meets), state, fade


def kernel(
    n_sp, n_tp, units,
    wv_ref, wg_ref, wc_ref, st_ref, out_ref0, meets_ref, gain_ref, skip_ref, proj_ref, blend_ref, taps_ref,
    mixed_ref,
    wbuf, stbuf, acc_state, heads, resid, nb, up, hid, psum, rbuf,
    own_sem, st_send, st_recv, z_send, z_recv, y_send, y_recv, h_send, h_recv, r_send, r_recv, n_send, n_recv, d_send, d_recv,
):
    s, t = lax.axis_index("sp"), lax.axis_index("tp")
    nz = n_sp // 2
    z, y = s // 2, s % 2
    q = z % 2
    mate = s + 2 - 4 * q
    side = s + 1 - 2 * y
    tok = skip_ref.shape[0]
    cols = skip_ref.shape[1]
    half = wbuf.shape[2]
    dblk = wbuf.shape[3]
    dv = out_ref0.shape[1] // units

    def rc(src, dst, ss, rs, sp, tp):
        return pltpu.make_async_remote_copy(
            src_ref=src, dst_ref=dst, send_sem=ss, recv_sem=rs,
            device_id=(sp, tp), device_id_type=pl.DeviceIdType.MESH,
        )

    bar = pltpu.get_barrier_semaphore()
    count = 0
    for o in range(1, n_sp):
        pl.semaphore_signal(bar, inc=1, device_id=(lax.rem(s + o, n_sp), t),
                            device_id_type=pl.DeviceIdType.MESH)
        count += 1
    for row in (s, mate):
        for o in range(1, n_tp):
            pl.semaphore_signal(bar, inc=1, device_id=(row, lax.rem(t + o, n_tp)),
                                device_id_type=pl.DeviceIdType.MESH)
            count += 1
    pl.semaphore_wait(bar, count)

    st = [None] + [
        rc(st_ref, stbuf.at[s], st_send.at[o], st_recv.at[o], lax.rem(s + o, n_sp), t)
        for o in range(1, n_sp)
    ]
    for o in range(1, n_sp):
        @pl.when(s + o < n_sp)
        def _(o=o):
            st[o].start()

    w_refs = (wv_ref, wg_ref, wc_ref)
    my_rows = pl.ds(pl.multiple_of(q * half, HALO), half)
    slots = [s] + [lax.rem(z + nz - o, nz) * 2 + y for o in range(1, nz)]
    side_slots = [slot + 1 - 2 * y for slot in slots]
    zc, yc = [], []
    for m in range(3):
        made = [None]
        for o in range(1, nz):
            zz = lax.rem(z + o, nz)
            rows = pl.ds(pl.multiple_of((zz % 2) * half, HALO), half)
            made.append(rc(w_refs[m].at[rows], wbuf.at[s, m], z_send.at[m, o], z_recv.at[m, o],
                           zz * 2 + y, t))
        zc.append(made)
        yc.append([
            rc(w_refs[m].at[my_rows] if o == 0 else wbuf.at[slots[o], m], wbuf.at[slots[o], m],
               y_send.at[m, o], y_recv.at[m, o], side, t)
            for o in range(nz)
        ])

    def forward(m, o):
        zc[m][o].wait_recv()
        yc[m][o].start()

    for o in range(1, nz):
        zc[0][o].start()
        zc[1][o].start()
    for m in range(3):
        yc[m][0].start()
    owns = [
        pltpu.make_async_copy(w_refs[m].at[my_rows], wbuf.at[s, m], own_sem.at[m])
        for m in range(3)
    ]
    for copy in owns:
        copy.start()

    acc_state[...] = jnp.zeros_like(acc_state)
    for o in range(n_sp - 1, 0, -1):
        @pl.when(s - o >= 0)
        def _(o=o):
            st[o].wait_recv()
            got = stbuf[s - o].astype(F32)
            acc_state[...] = got[dv : dv + 1] * acc_state[...] + got[:dv]
    key = meets_ref.shape[1] // units
    mine = []
    for u in range(units):
        total = out_ref0[:, u * dv : (u + 1) * dv] + lax.dot_general(
            meets_ref[:, u * key : (u + 1) * key], acc_state[:, u * key : (u + 1) * key],
            NT, precision=HIGHEST, preferred_element_type=F32,
        )
        scale = lax.rsqrt(jnp.mean(total * total, axis=-1, keepdims=True) + EPSILON)
        mine.append((total * scale * gain_ref[u : u + 1, :]).astype(BF16))
    heads[t] = jnp.concatenate(mine, axis=1)
    hc = [
        rc(heads.at[t], heads.at[t], h_send.at[o], h_recv.at[o], s, lax.rem(t + o, n_tp))
        for o in range(1, n_tp)
    ]
    for copy in hc:
        copy.start()
    for copy in hc:
        copy.wait_recv()
    width = units * dv
    projected = skip_ref[...].astype(F32)
    whole_heads = jnp.concatenate([heads[i] for i in range(n_tp)], axis=1)
    projected = projected + jnp.dot(whole_heads, proj_ref[...], preferred_element_type=F32)
    resid[t] = projected.astype(BF16)
    qc = [
        rc(resid.at[t], resid.at[t], r_send.at[o], r_recv.at[o], s, lax.rem(t + o, n_tp))
        for o in range(1, n_tp)
    ]
    for copy in qc:
        copy.start()
    for copy in qc:
        copy.wait_recv()
    squares = jnp.zeros((tok, 1), F32)
    for i in range(n_tp):
        part = resid[i].astype(F32)
        squares = squares + jnp.sum(part * part, axis=1, keepdims=True)
    scale = lax.rsqrt(squares / (n_tp * cols) + EPSILON)
    for i in range(n_tp):
        piece = slice(i * cols, (i + 1) * cols)
        nb[0, HALO:, piece] = (
            resid[i].astype(F32) * scale * blend_ref[:, piece]
        ).astype(BF16)
    if nz > 1:
        forward(0, 1)
        forward(1, 1)
    after = lax.rem(s + 1, n_sp)
    after_mate = after + 2 - 4 * ((after // 2) % 2)
    block = pl.ds(HALO, tok)
    tail = pl.ds(tok, HALO)
    nc = [
        rc(nb.at[0, tail], nb.at[0, pl.ds(0, HALO)], n_send.at[0], n_recv.at[0], after, t),
        rc(nb.at[0, tail], nb.at[1, pl.ds(0, HALO)], n_send.at[1], n_recv.at[1], after_mate, t),
        rc(nb.at[0, block], nb.at[1, block], n_send.at[2], n_recv.at[2], mate, t),
    ]
    for copy in nc:
        copy.start()
    for o in range(1, nz):
        zc[2][o].start()
    for m in range(2):
        for i in range(2):
            up[m, i] = jnp.zeros_like(up[m, i])
    for copy in nc:
        copy.wait_recv()
    for copy in owns:
        copy.wait()
    if dblk % 128 == 0:

        def expand(b):
            at = pl.ds(pl.multiple_of(b * dblk, 128), dblk)
            for i in range(2):
                rows = nb[i, :, at]
                for m in range(2):
                    up[m, i] += lax.dot_general(
                        rows, wbuf[b, m], NT, preferred_element_type=F32
                    )

        for o in range(nz):
            if o > 1:
                forward(0, o)
                forward(1, o)
            expand(slots[o])
        for o in range(nz):
            if o == nz - 1:
                forward(2, 1)
            yc[0][o].wait_recv()
            yc[1][o].wait_recv()
            expand(side_slots[o])
        for o in range(2, nz):
            forward(2, o)
    else:
        for o in range(2, nz):
            forward(0, o)
            forward(1, o)
        for o in range(nz):
            yc[0][o].wait_recv()
            yc[1][o].wait_recv()
        group = 128 // dblk

        def expand_some(b, carry):
            at = pl.ds(pl.multiple_of(b * group * dblk, 128), group * dblk)
            for i in range(2):
                rows = nb[i, :, at]
                for j in range(group):
                    part = rows[:, j * dblk : (j + 1) * dblk]
                    for m in range(2):
                        up[m, i] += lax.dot_general(
                            part, wbuf[b * group + j, m], NT, preferred_element_type=F32
                        )
            return carry

        lax.fori_loop(0, n_sp // group, expand_some, 0)
        for o in range(1, nz):
            forward(2, o)
    for i in range(2):
        first = (s if i == 0 else mate) == 0
        conv = []
        for m in range(2):
            keep = jnp.where(first, 0.0, 1.0)
            edge = up[m, i, :HALO].astype(BF16).astype(F32)
            up[m, i, :HALO] = edge * keep
            up[m, i, HALO:] = up[m, i, HALO:].astype(BF16).astype(F32)
            total = taps_ref[m * 3 : m * 3 + 1] * up[m, i, pl.ds(HALO - 2, tok)]
            total += taps_ref[m * 3 + 1 : m * 3 + 2] * up[m, i, pl.ds(HALO - 1, tok)]
            total += taps_ref[m * 3 + 2 : m * 3 + 3] * up[m, i, pl.ds(HALO, tok)]
            conv.append(total)
        value, gate = conv
        hid[pl.ds(i * tok, tok)] = (gate / (1.0 + jnp.exp(-gate)) * value).astype(BF16)
    per = cols // dblk
    if dblk % 128 == 0:

        def share(b, i):
            return rc(psum.at[b, i], rbuf.at[i * n_tp + t, b % per], d_send.at[b, i],
                      d_recv.at[i * n_tp + t, b % per], s if i == 0 else mate, b // per)

        for k in range(n_sp):
            b = slots[k] if k < nz else side_slots[k - nz]
            if k >= nz:
                yc[2][k - nz].wait_recv()
            part = jnp.dot(hid[...], wbuf[b, 2], preferred_element_type=F32).astype(BF16)
            psum[b, 1] = part[tok:]
            share(b, 1).start()
            psum[b, 0] = part[:tok]

            @pl.when(b // per != t)
            def _(b=b):
                share(b, 0).start()

        sums = []
        for j in range(per):
            total = resid[t, :, j * dblk : (j + 1) * dblk].astype(F32)
            total = total + psum[t * per + j, 0].astype(F32)
            for i in range(2):
                for o in range(1, n_tp + i):
                    at = i * n_tp + lax.rem(t + o, n_tp)
                    rc(psum.at[0, 0], rbuf.at[at, j], d_send.at[0, 0], d_recv.at[at, j],
                       s if i == 0 else mate, lax.rem(t + o, n_tp) if i == 0 else t).wait_recv()
                    total = total + rbuf[at, j].astype(F32)
            sums.append(total.astype(BF16))
        mixed_ref[...] = jnp.concatenate(sums, axis=1)
        for k in range(n_sp):
            b = slots[k] if k < nz else side_slots[k - nz]
            share(b, 1).wait_send()

            @pl.when(b // per != t)
            def _(b=b):
                share(b, 0).wait_send()
        dc = []
    else:
        for o in range(nz):
            yc[2][o].wait_recv()
        dc = []
        for o in range(1, n_tp + 1):
            to = lax.rem(t + o, n_tp)
            for j in range(per):
                part = jnp.dot(
                    hid[...], wbuf[to * per + j, 2], preferred_element_type=F32
                ).astype(BF16)
                psum[to, 0, :, j * dblk : (j + 1) * dblk] = part[:tok]
                psum[to, 1, :, j * dblk : (j + 1) * dblk] = part[tok:]
            for i in range(2):
                if i == 0 and o == n_tp:
                    continue
                at = i * n_tp + o - 1
                copy = rc(psum.at[to, i], rbuf.at[at], d_send.at[at, 0], d_recv.at[at, 0],
                          s if i == 0 else mate, to)
                copy.start()
                dc.append((at, copy))
        total = psum[t, 0].astype(F32)
        for at, copy in dc:
            copy.wait_recv()
            total = total + rbuf[at].astype(F32)
        mixed_ref[...] = (resid[t].astype(F32) + total).astype(BF16)

    for o in range(1, n_sp):
        @pl.when(s + o < n_sp)
        def _(o=o):
            st[o].wait_send()
    for m in range(3):
        for copy in zc[m][1:] + yc[m]:
            copy.wait_send()
    for copy in hc + qc + nc + [c for _, c in dc]:
        copy.wait_send()


def local(
    n_sp, n_tp,
    skip_stream,
    narrow_lookup_matrix,
    narrow_probe_matrix,
    narrow_retention_logits,
    broad_lookup_matrix,
    broad_probe_matrix,
    broad_retention_logits,
    content_vectors,
    extra_log_retention,
    per_branch_scaling,
    final_projection_matrix,
    channel_blend_scaling,
    switch_expansion_matrix,
    content_expansion_matrix,
    convolution_kernel,
    contraction_matrix,
):
    tok, cols = skip_stream.shape
    heads = content_vectors.shape[1]
    dv = content_vectors.shape[3]
    narrow = narrow_lookup_matrix.shape[1] // heads
    broad = broad_lookup_matrix.shape[1] // heads
    units = 2 * heads

    def pair(a, b):
        a = a.astype(F32).reshape(tok, heads, narrow)
        b = b.astype(F32).reshape(tok, heads, broad)
        return a, b

    def join(a, b):
        a = jnp.pad(a, ((0, 0), (0, 0), (0, broad - narrow)))
        return jnp.stack([a, b], axis=2).reshape(tok, units, broad)

    qa, qb = pair(narrow_lookup_matrix, broad_lookup_matrix)
    query = join(qa * narrow ** (-0.5), qb * broad ** (-0.5))
    keys = join(*pair(narrow_probe_matrix, broad_probe_matrix))
    gates = join(*pair(narrow_retention_logits, broad_retention_logits))
    extra = extra_log_retention.transpose(0, 2, 1).reshape(tok, units, 1)
    decay = jax.nn.log_sigmoid(gates) / SOFTENING + extra
    values = content_vectors.astype(F32).reshape(tok, units, dv)
    out, meets, state, fade = local_attention(query, keys, values, decay)
    packed = jnp.concatenate(
        [
            state.transpose(1, 0, 2).reshape(dv, units * broad),
            fade.reshape(1, units * broad),
            jnp.zeros((15, units * broad), F32),
        ],
        axis=0,
    ).astype(BF16)
    ff = contraction_matrix.shape[0]
    half = ff // 2
    dblk = contraction_matrix.shape[1]
    q = (lax.axis_index("sp") // 2) % 2
    taps = lax.dynamic_slice_in_dim(convolution_kernel, q * half, half, axis=2)
    taps = jnp.pad(taps.astype(F32).transpose(1, 0, 2).reshape(6, half), ((0, 2), (0, 0)))
    gain = per_branch_scaling.astype(F32).reshape(units, dv)
    blend = channel_blend_scaling.astype(F32).reshape(1, -1)
    nz = n_sp // 2
    model = n_tp * cols
    dma = pltpu.SemaphoreType.DMA
    per = cols // dblk
    if dblk % 128 == 0:
        shares = (
            pltpu.VMEM((n_sp, 2, tok, dblk), BF16),
            pltpu.VMEM((2 * n_tp, per, tok, dblk), BF16),
        )
        sent, got = (n_sp, 2), (2 * n_tp, per)
    else:
        shares = (
            pltpu.VMEM((n_tp, 2, tok, cols), BF16),
            pltpu.VMEM((2 * n_tp, tok, cols), BF16),
        )
        sent, got = (2 * n_tp, 1), (2 * n_tp, 1)
    vmem = pl.BlockSpec(memory_space=pltpu.VMEM)
    return pl.pallas_call(
        functools.partial(kernel, n_sp, n_tp, units),
        out_shape=jax.ShapeDtypeStruct((tok, cols), BF16),
        in_specs=[vmem] * 11,
        out_specs=vmem,
        scratch_shapes=[
            pltpu.VMEM((n_sp, 3, half, dblk), BF16),
            pltpu.VMEM((n_sp,) + packed.shape, BF16),
            pltpu.VMEM((dv, units * broad), F32),
            pltpu.VMEM((n_tp, tok, units * dv), BF16),
            pltpu.VMEM((n_tp, tok, cols), BF16),
            pltpu.VMEM((2, tok + HALO, model), BF16),
            pltpu.VMEM((2, 2, tok + HALO, half), F32),
            pltpu.VMEM((2 * tok, half), BF16),
            *shares,
            dma((3,)),
            dma((n_sp,)), dma((n_sp,)),
            dma((3, nz)), dma((3, nz)), dma((3, nz)), dma((3, nz)),
            dma((n_tp,)), dma((n_tp,)), dma((n_tp,)), dma((n_tp,)),
            dma((3,)), dma((3,)), dma(sent), dma(got),
        ],
        compiler_params=pltpu.CompilerParams(
            collective_id=0, has_side_effects=True, vmem_limit_bytes=56 * 1024 * 1024
        ),
    )(content_expansion_matrix.T, switch_expansion_matrix.T, contraction_matrix, packed, out, meets, gain, skip_stream, final_projection_matrix, blend, taps)


def solution(mesh):
    in_specs = (
        P("sp", "tp"),
        P("sp", "tp"),
        P("sp", "tp"),
        P("sp", "tp"),
        P("sp", "tp"),
        P("sp", "tp"),
        P("sp", "tp"),
        P("sp", "tp", None, None),
        P("sp", None, "tp"),
        P("tp", None, None),
        P(None, "tp"),
        P(),
        P("sp", "tp"),
        P("sp", "tp"),
        P(None, None, "tp"),
        P("tp", "sp"),
    )
    out_specs = P("sp", "tp")
    body = functools.partial(local, mesh.shape["sp"], mesh.shape["tp"])
    return jax.shard_map(body, mesh=mesh, in_specs=in_specs, out_specs=out_specs, check_vma=False)
```
